32 devices in a mesh: ep: 32 (over z, y, x, core).
Axes of the slice: x: 2, y: 2, z: 4, core: 2. Of those that a mesh axis runs over, the one named last changes fastest.
Arguments:
- tokens: bfloat16 [640, 2048], P('ep'), may hold values from -6 to 6
- positions: int32 [640], P('ep'), may hold values from 1024 to 16383
- state: float32 [640, 8, 64, 128], P('ep'), may hold values from -1.6 to 1.6
- mix_gain: float32 [2048], replicated, may hold values from 0.1 to 1.9
- w_query: bfloat16 [2048, 512], replicated, may hold values from -0.125 to 0.125
- w_key: bfloat16 [2048, 512], replicated, may hold values from -0.125 to 0.125
- w_value: bfloat16 [2048, 1024], replicated, may hold values from -0.125 to 0.125
- ret_gain: float32 [1024], replicated, may hold values from 0.1 to 1.9
- w_out: bfloat16 [1024, 2048], P(None, 'ep'), may hold values from -0.1875 to 0.1875
- ffn_gain: float32 [2048], replicated, may hold values from 0.1 to 1.9
- routes: int32 [640, 6], P('ep'), may hold values from 0 to 31, all different within a row; in each aligned block of 20 rows (0 to 19, 20 to 39, ...) at most 7 rows name the same one
- route_weights: float32 [640, 6], P('ep'), may hold values from 0.1 to 1
- expert_gate: bfloat16 [32, 2048, 512], P('ep'), may hold values from -0.125 to 0.125
- expert_up: bfloat16 [32, 2048, 512], P('ep'), may hold values from -0.125 to 0.125
- expert_down: bfloat16 [32, 512, 2048], P('ep'), may hold values from -0.25 to 0.25
Outputs:
- result: bfloat16 [640, 2048], P('ep')
- new_state: float32 [640, 8, 64, 128], P('ep')
The draws below stay inside these ranges and needn't reach their ends.
Inputs may be any that keep to these rules, and one draw needn't show every extreme that they name: `routes`: each row names 6 different experts; among the rows of one device no expert is named more than 7 times, a bound that some block reaches there.
All inputs are finite; a program needn't handle non-finite values.
Results may differ from the reference program's by a relative error of at most 0.017.
Values may be sent and summed in bfloat16 or wider, within the bound.
A program may use at most 128 MiB of HBM per device.

```python
import math
import jax
import jax.numpy as jnp
import numpy as np
from jax import lax

D = 2048
HEADS = 8
HEAD_K = 64
HEAD_V = 128
FE = 512
TOPK = 6
SEQ_DEV = 20
QK = 512
VW = 1024
EXPERTS = 32
CAP = 7
TOKENS = 640
N_EP = 32


def touch_ends(values, own_key, smallest, top_value):
    longest = values.shape.index(max(values.shape))
    spots = []
    for shift in (0, 1):
        where = [jax.random.randint(jax.random.fold_in(own_key, axis), (), 0, length) for axis, length in enumerate(values.shape)]
        where[longest] = (where[longest] + shift) % values.shape[longest]
        spots.append(tuple(where))
    return values.at[spots[0]].set(smallest).at[spots[1]].set(top_value)


def shard_levels(rng, extent, pieces, smallest, high):
    level = 1.0
    for dim, blocks in pieces:
        heights = jax.random.uniform(jax.random.fold_in(jax.random.fold_in(rng, 6), dim), (blocks,), jnp.float32, smallest / len(pieces), high / len(pieces))
        level = level * jnp.repeat(jnp.exp(heights), extent[dim] // blocks).reshape((-1,) + (1,) * (len(extent) - 1 - dim))
    return level


def assign_block(stream_key, own, number, rows, count, top, bound, skew):
    order = jax.random.permutation(stream_key, count)
    crowded, common = portions_of(count, rows * top, bound, skew, True), portions_of(count, rows * top, bound, skew, False)
    places = jnp.arange(count)

    def named(sizes, rotation):
        used = int((sizes > 0).sum())
        fixed = max(1, used // 4)
        passed = fixed + (places - fixed + rotation * (used - fixed)) % max(1, count - fixed)
        return jnp.zeros((count,), jnp.int32).at[order[jnp.where(places < fixed, places, passed)]].set(jnp.asarray(sizes, jnp.int32))

    sizes = jnp.where(number % 4 == 0, named(crowded, number // 4), named(common, number - number // 4 - 1))
    mixed = jax.random.permutation(jax.random.fold_in(own, 3), count)
    donor, receiver = mixed[0:count // 2 * 2:2], mixed[1:count // 2 * 2:2]
    margin = jnp.minimum(sizes[donor] - 1, bound - sizes[receiver]) // 2
    margin = jnp.where((donor == order[0]) | (receiver == order[0]) | (sizes[receiver] == 0), 0, jnp.maximum(margin, 0))
    passed = jax.random.randint(jax.random.fold_in(own, 4), (count // 2,), 0, 1 << 20) % (margin + 1)
    sizes = sizes.at[donor].add(-passed).at[receiver].add(passed)
    items = jnp.searchsorted(jnp.cumsum(sizes), jnp.arange(rows * top), side="right").astype(jnp.int32)
    listing = items.reshape(top, rows).T
    listing = listing[jax.random.permutation(jax.random.fold_in(own, 1), rows)]
    rotation = jax.random.randint(jax.random.fold_in(own, 2), (rows, 1), 0, top)
    return jnp.take_along_axis(listing, (jnp.arange(top)[None, :] + rotation) % top, axis=1)


def portions_of(amount, total, limit, lean, full):
    weights = [(1 << 20) // math.isqrt(standing ** lean) + 1 for standing in range(1, amount + 1)]
    largest = limit if full else min(limit, max(-(-total // amount), total * weights[0] // sum(weights)))
    least = 1 if total - largest >= amount - 1 else 0
    given, spare = [largest] + [least] * (amount - 1), total - largest - least * (amount - 1)
    while spare > 0:
        free = [i for i in range(1, amount) if given[i] < largest] or [i for i in range(1, amount) if given[i] < limit]
        mass, remaining = sum([weights[i] for i in free]), spare
        for i in free:
            extra = min(limit - given[i], max(1, remaining * weights[i] // mass), spare)
            given[i] = given[i] + extra
            spare = spare - extra
    return np.array(given)


def bell_draw(key, shape, spread, reach, cuts=(), held_as=jnp.bfloat16):
    values = jax.random.normal(key, shape, jnp.float32) * spread
    if len(cuts) > 0:
        values = shard_levels(key, shape, cuts, -0.22, 0.18) * values
    return jnp.clip(values, min=-reach, max=reach).astype(held_as)


def setup_inputs(seed: int = 0) -> dict:
    key_list = jax.random.split(jax.random.key(seed), 16)
    tokens = bell_draw(key_list[0], (TOKENS, D), 1.0, 6.0, ((0, 32),))
    positions = touch_ends(jax.random.randint(key_list[1], (TOKENS,), 1024, 16384), jax.random.fold_in(key_list[1], 1), 1024, 16383).astype(jnp.int32)
    state = bell_draw(key_list[2], (TOKENS, HEADS, HEAD_K, HEAD_V), 0.2, 1.6, ((0, 32),), jnp.float32)
    mix_gain = jnp.clip(1.0 + 0.18 * jax.random.normal(key_list[3], (D,), jnp.float32), 0.1, 1.9)
    w_query = bell_draw(key_list[4], (D, QK), D ** -0.5, 0.125)
    w_key = bell_draw(key_list[5], (D, QK), D ** -0.5, 0.125)
    w_value = bell_draw(key_list[6], (D, VW), D ** -0.5, 0.125)
    ret_gain = jnp.clip(1.0 + 0.18 * jax.random.normal(key_list[7], (VW,), jnp.float32), 0.1, 1.9)
    w_out = bell_draw(key_list[8], (VW, D), VW ** -0.5, 0.1875, ((1, 32),))
    ffn_gain = jnp.clip(1.0 + 0.18 * jax.random.normal(key_list[9], (D,), jnp.float32), 0.1, 1.9)
    routes_keys = jax.random.split(jax.random.fold_in(key_list[10], 1), TOKENS // SEQ_DEV)
    routes_turns = jax.random.permutation(jax.random.fold_in(key_list[10], 3), TOKENS // SEQ_DEV)
    routes = jax.vmap(lambda own, number: assign_block(jax.random.fold_in(key_list[10], 2), own, number, SEQ_DEV, EXPERTS, TOPK, CAP, 1))(routes_keys, routes_turns).reshape((TOKENS, TOPK))
    route_weights = jnp.clip(0.1 + 0.9 * jax.random.uniform(key_list[11], (TOKENS, TOPK), jnp.float32) ** shard_levels(key_list[11], (TOKENS, TOPK), ((0, 32),), -0.2, 0.2), 0.1, 1.0)
    expert_gate = bell_draw(key_list[12], (EXPERTS, D, FE), D ** -0.5, 0.125, ((0, 32),))
    expert_up = bell_draw(key_list[13], (EXPERTS, D, FE), D ** -0.5, 0.125, ((0, 32),))
    expert_down = bell_draw(key_list[14], (EXPERTS, FE, D), FE ** -0.5, 0.25, ((0, 32),))
    return {"tokens": tokens, "positions": positions, "state": state, "mix_gain": mix_gain, "w_query": w_query, "w_key": w_key, "w_value": w_value, "ret_gain": ret_gain, "w_out": w_out, "ffn_gain": ffn_gain, "routes": routes, "route_weights": route_weights, "expert_gate": expert_gate, "expert_up": expert_up, "expert_down": expert_down}


EPS = 1e-06

def rms_scale(values, gain):
    wide = values.astype(jnp.float32)
    scaled = wide * lax.rsqrt(lax.optimization_barrier(jnp.mean(wide * wide, axis=-1, keepdims=True)) + EPS)
    return (scaled * gain.astype(jnp.float32)).astype(jnp.bfloat16)

def rotate(field, spots):
    half = field.shape[-1] // 2
    freqs = jnp.exp(-math.log(10000.0) * jnp.arange(half, dtype=jnp.float32) / half)
    angle = spots.astype(jnp.float32)[:, None] * freqs[None, :]
    cosine = jnp.cos(angle)[:, None, :]
    sine = jnp.sin(angle)[:, None, :]
    first = field[..., :half]
    second = field[..., half:]
    return jnp.concatenate([first * cosine - second * sine, second * cosine + first * sine], axis=-1)

def reference(tokens, positions, state, mix_gain, w_query, w_key, w_value, ret_gain, w_out, ffn_gain, routes, route_weights, expert_gate, expert_up, expert_down):
    normed_in = rms_scale(tokens, mix_gain)
    q_proj = jnp.dot(normed_in, w_query, preferred_element_type=jnp.float32).astype(jnp.bfloat16)
    k_proj = jnp.dot(normed_in, w_key, preferred_element_type=jnp.float32).astype(jnp.bfloat16)
    v_proj = jnp.dot(normed_in, w_value, preferred_element_type=jnp.float32).astype(jnp.bfloat16)
    queries = rotate(q_proj.astype(jnp.float32).reshape(TOKENS, HEADS, HEAD_K), positions)
    key_rows = rotate(k_proj.astype(jnp.float32).reshape(TOKENS, HEADS, HEAD_K), positions) * HEAD_K ** (-0.5)
    values = v_proj.astype(jnp.float32).reshape(TOKENS, HEADS, HEAD_V)
    decays = 1.0 - jnp.exp2(-2.0 - jnp.arange(HEADS, dtype=jnp.float32))
    new_state = decays[None, :, None, None] * state + key_rows[:, :, :, None] * values[:, :, None, :]
    readout = jnp.einsum('thd,thdv->thv', queries, new_state, precision=lax.Precision.HIGHEST)
    centre = lax.optimization_barrier(jnp.mean(readout, axis=-1, keepdims=True))
    variance = lax.optimization_barrier(jnp.mean(jnp.square(readout - centre), axis=-1, keepdims=True))
    normed = ((readout - centre) * lax.rsqrt(variance + EPS)).reshape(TOKENS, VW) * ret_gain
    mixed = normed.astype(jnp.bfloat16)
    attended = jnp.dot(mixed, w_out, preferred_element_type=jnp.float32).astype(jnp.bfloat16)
    resid = (tokens.astype(jnp.float32) + attended.astype(jnp.float32)).astype(jnp.bfloat16)
    normed_mid = rms_scale(resid, ffn_gain)
    per_dev = SEQ_DEV * TOPK
    chosen = routes.reshape(N_EP, per_dev).astype(jnp.int32)
    matches = (chosen[:, :, None] == jnp.arange(EXPERTS, dtype=jnp.int32)[None, None, :]).astype(jnp.int32)
    places = lax.optimization_barrier(jnp.sum((jnp.cumsum(matches, axis=1) - matches) * matches, axis=-1))
    dev_ids = jnp.arange(N_EP, dtype=jnp.int32)[:, None]
    targets = (chosen * (N_EP * CAP) + dev_ids * CAP + places).reshape(-1).astype(jnp.int32)
    row_ids = jnp.arange(TOKENS * TOPK, dtype=jnp.int32)
    table = jnp.full((EXPERTS * N_EP * CAP,), -1, jnp.int32).at[targets].set(row_ids)
    table = table.reshape(EXPERTS, N_EP * CAP)

    def serve(items):
        gate_w, up_w, down_w, ids = items
        picked = jnp.where(ids[:, None] >= 0, normed_mid[jnp.maximum(ids, 0) // TOPK], jnp.zeros((), jnp.bfloat16))
        picked = picked.astype(jnp.bfloat16)
        gate_part = jnp.dot(picked, gate_w, preferred_element_type=jnp.float32)
        up_part = jnp.dot(picked, up_w, preferred_element_type=jnp.float32)
        hidden = (jax.nn.silu(gate_part) * up_part).astype(jnp.bfloat16)
        return jnp.dot(hidden, down_w, preferred_element_type=jnp.float32).astype(jnp.bfloat16)
    outputs = lax.map(serve, (expert_gate, expert_up, expert_down, table))
    picked_rows = outputs.reshape(-1, D)[targets].astype(jnp.float32)
    mixture = lax.optimization_barrier(jnp.sum(picked_rows.reshape(TOKENS, TOPK, D) * route_weights[:, :, None], axis=1))
    result = (resid.astype(jnp.float32) + mixture).astype(jnp.bfloat16)
    return (result, new_state)
```

```python
import functools
import math

import jax
import jax.numpy as jnp
from jax import lax
from jax.experimental import pallas as pl
from jax.experimental.pallas import tpu as pltpu
from jax.sharding import PartitionSpec as P

EPS = 1e-06
MESH = pl.DeviceIdType.MESH
PAD = 8
VMEM_LIMIT = 64 * 1024 * 1024 - 128 * 1024


def layout_of(mesh):
    devices = list(mesh.devices.flat)
    count = len(devices)
    try:
        far = [max(d.coords[i] for d in devices) - min(d.coords[i] for d in devices) + 1 for i in range(3)]
        cores = count // (far[0] * far[1] * far[2])
        if cores * far[0] * far[1] * far[2] == count and cores >= 1:
            return (far[2], far[1], far[0], cores)
    except (AttributeError, TypeError, IndexError):
        pass
    cores = 2 if count % 2 == 0 else 1
    chips = count // cores
    side = 1
    while (side * 2) ** 2 * 4 <= chips and chips % ((side * 2) ** 2) == 0:
        side *= 2
    return (chips // (side * side), side, side, cores)


class Place:
    def __init__(self, dims):
        self.dims = dims
        depth, rows, cols, cores = dims
        me = lax.axis_index("ep")
        self.me = me
        self.spot = (
            me // (rows * cols * cores),
            (me // (cols * cores)) % rows,
            (me // cores) % cols,
            me % cores,
        )

    def at(self, dz, dy, dx, dc=0):
        total = 0
        for size, here, move in zip(self.dims, self.spot, (dz, dy, dx, dc)):
            total = total * size + (here + move) % size if move % size else total * size + here
        return total

    def greet(self):
        depth, rows, cols, cores = self.dims
        moves = [(d, 0, 0, 0) for d in range(1, depth)]
        moves += [(0, d, 0, 0) for d in range(1, rows)]
        moves += [(0, 0, d, 0) for d in range(1, cols)]
        moves += [(0, 0, 0, d) for d in range(1, cores)]
        barrier = pltpu.get_barrier_semaphore()
        for move in moves:
            pl.semaphore_signal(barrier, inc=1, device_id=(self.at(*move),), device_id_type=MESH)
        pl.semaphore_wait(barrier, len(moves))


def gather_names(dims):
    depth, rows, cols, cores = dims
    names = []
    for dz in range(depth):
        if dz:
            names.append(("z", dz, 0, 0, 0))
        for dx in range(1, cols):
            names.append(("x", dz, 0, dx, 0))
        for dy in range(1, rows):
            names.append(("y", dz, dy, 0, 0))
            for dx in range(1, cols):
                names.append(("p", dz, dy, dx, 0))
                names.append(("q", dz, dy, dx, 0))
        for dy in range(rows):
            for dx in range(cols):
                for dc in range(1, cores):
                    names.append(("c", dz, dy, dx, dc))
    return {name: i for i, name in enumerate(names)}


class Gather:
    def __init__(self, place, view, send, recv):
        self.place, self.view, self.send, self.recv = place, view, send, recv
        self.names = gather_names(place.dims)
        self.sent = []

    def copy(self, name):
        kind, dz, dy, dx, dc = name
        m = self.names[name]
        back = {"z": (-dz, 0, 0, 0), "x": (0, 0, -dx, 0), "y": (0, -dy, 0, 0)}
        back.update({"p": (0, -dy, 0, 0), "q": (0, 0, -dx, 0), "c": (0, 0, 0, -dc)})
        return m, {"p": 0, "q": 1}.get(kind), self.place.at(*back[kind])

    def put(self, name, held):
        m, half, target = self.copy(name)
        ref = self.view(self.place.at(*held), half)
        c = pltpu.make_async_remote_copy(
            src_ref=ref, dst_ref=ref, send_sem=self.send.at[m], recv_sem=self.recv.at[m],
            device_id=(target,), device_id_type=MESH,
        )
        c.start()
        self.sent.append(c)

    def get(self, name):
        m, half, target = self.copy(name)
        ref = self.view(self.place.at(*name[1:]), half)
        pltpu.make_async_remote_copy(
            src_ref=ref, dst_ref=ref, send_sem=self.send.at[m], recv_sem=self.recv.at[m],
            device_id=(target,), device_id_type=MESH,
        ).wait_recv()

    def mates(self, dz, dy, dx):
        for dc in range(1, self.place.dims[3]):
            self.put(("c", dz, dy, dx, dc), (dz, dy, dx, 0))

    def first(self, dz):
        depth, rows, cols, cores = self.place.dims
        if dz == 0:
            for d in range(1, depth):
                self.put(("z", d, 0, 0, 0), (0, 0, 0, 0))
        else:
            self.get(("z", dz, 0, 0, 0))
        for dx in range(1, cols):
            self.put(("x", dz, 0, dx, 0), (dz, 0, 0, 0))
        for dy in range(1, rows):
            self.put(("y", dz, dy, 0, 0), (dz, 0, 0, 0))
        self.mates(dz, 0, 0)

    def second(self, dz):
        depth, rows, cols, cores = self.place.dims
        for dx in range(1, cols):
            self.get(("x", dz, 0, dx, 0))
            for dy in range(1, rows):
                self.put(("p", dz, dy, dx, 0), (dz, 0, dx, 0))
            self.mates(dz, 0, dx)
        for dy in range(1, rows):
            self.get(("y", dz, dy, 0, 0))
            for dx in range(1, cols):
                self.put(("q", dz, dy, dx, 0), (dz, dy, 0, 0))
            self.mates(dz, dy, 0)

    def third(self, dz):
        depth, rows, cols, cores = self.place.dims
        for dy in range(1, rows):
            for dx in range(1, cols):
                self.get(("p", dz, dy, dx, 0))
                self.get(("q", dz, dy, dx, 0))
                self.mates(dz, dy, dx)

    def fourth(self, dz):
        depth, rows, cols, cores = self.place.dims
        for dy in range(rows):
            for dx in range(cols):
                for dc in range(1, cores):
                    self.get(("c", dz, dy, dx, dc))

    def finish(self):
        for c in self.sent:
            c.wait_send()


def halves(ref, width):
    cut = -(-width // 256) * 128
    spans = {None: (0, width), 0: (0, cut), 1: (cut, width - cut)}

    def view(index, half):
        start, size = spans[half]
        return ref.at[index, :, pl.ds(start, size)]

    return view


def gather_kernel(dims, own, out, load, send, recv):
    place = Place(dims)
    fill = pltpu.make_async_copy(own, out.at[place.me], load)
    fill.start()
    place.greet()
    fill.wait()
    g = Gather(place, halves(out, out.shape[2]), send, recv)
    depth = dims[0]
    for t in range(depth + 3):
        if t < depth:
            g.first(t)
        if 0 <= t - 1 < depth:
            g.second(t - 1)
        if 0 <= t - 2 < depth:
            g.third(t - 2)
        if 0 <= t - 3 < depth:
            g.fourth(t - 3)
    g.finish()


def gather_blocks(dims, block, collective):
    count = math.prod(dims)
    messages = len(gather_names(dims))
    return pl.pallas_call(
        functools.partial(gather_kernel, dims),
        out_shape=jax.ShapeDtypeStruct((count,) + block.shape, block.dtype),
        in_specs=[pl.BlockSpec(memory_space=pl.ANY)],
        out_specs=pl.BlockSpec(memory_space=pltpu.VMEM),
        scratch_shapes=[
            pltpu.SemaphoreType.DMA,
            pltpu.SemaphoreType.DMA((messages,)),
            pltpu.SemaphoreType.DMA((messages,)),
        ],
        compiler_params=pltpu.CompilerParams(
            collective_id=collective, has_side_effects=True, vmem_limit_bytes=VMEM_LIMIT
        ),
        name="gather_blocks",
    )(block)


class Reduce:
    def __init__(self, place, parts, slots, send, recv):
        self.place, self.parts, self.slots, self.send, self.recv = place, parts, slots, send, recv
        self.names = gather_names(place.dims)
        self.sent = []
        self.width = parts.shape[2]

    def span(self, half):
        cut = self.width // 2
        return {None: pl.ds(0, self.width), 0: pl.ds(0, cut), 1: pl.ds(cut, self.width - cut)}[half]

    def copy(self, name):
        kind, dz, dy, dx, dc = name
        m = self.names[name]
        ahead = {"z": (dz, 0, 0, 0), "x": (0, 0, dx, 0), "y": (0, dy, 0, 0)}
        ahead.update({"p": (0, dy, 0, 0), "q": (0, 0, dx, 0), "c": (0, 0, 0, dc)})
        cols = self.span({"p": 0, "q": 1}.get(kind))
        return pltpu.make_async_remote_copy(
            src_ref=self.parts.at[self.place.at(dz, dy, dx, dc), :, cols],
            dst_ref=self.slots.at[m, :, cols],
            send_sem=self.send.at[m], recv_sem=self.recv.at[m],
            device_id=(self.place.at(*ahead[kind]),), device_id_type=MESH,
        )

    def put(self, name):
        c = self.copy(name)
        c.start()
        self.sent.append(c)

    def get(self, name):
        kind = name[0]
        self.copy(name).wait_recv()
        cols = self.span({"p": 0, "q": 1}.get(kind))
        return self.slots[self.names[name], :, cols].astype(jnp.float32)

    def add(self, index, cols, terms):
        value = self.parts[index, :, cols].astype(jnp.float32)
        for term in terms:
            value = value + term
        self.parts[index, :, cols] = value.astype(self.parts.dtype)

    def zeroth(self, dz):
        depth, rows, cols, cores = self.place.dims
        order = sorted(((dy, dx) for dy in range(rows) for dx in range(cols)), key=lambda o: (not o[0]) + (not o[1]))
        for dy, dx in order:
            for dc in range(1, cores):
                self.put(("c", dz, dy, dx, dc))

    def first(self, dz):
        depth, rows, cols, cores = self.place.dims
        order = sorted(((dy, dx) for dy in range(rows) for dx in range(cols)), key=lambda o: (not o[0]) + (not o[1]))
        for dy, dx in order:
            terms = [self.get(("c", dz, dy, dx, dc)) for dc in range(1, cores)]
            if terms:
                self.add(self.place.at(dz, dy, dx), self.span(None), terms)
            if dy and dx:
                self.put(("p", dz, dy, dx, 0))
                self.put(("q", dz, dy, dx, 0))

    def second(self, dz):
        depth, rows, cols, cores = self.place.dims
        for dx in range(1, cols):
            terms = [self.get(("p", dz, dy, dx, 0)) for dy in range(1, rows)]
            if terms:
                self.add(self.place.at(dz, 0, dx), self.span(0), terms)
            self.put(("x", dz, 0, dx, 0))
        for dy in range(1, rows):
            terms = [self.get(("q", dz, dy, dx, 0)) for dx in range(1, cols)]
            if terms:
                self.add(self.place.at(dz, dy, 0), self.span(1), terms)
            self.put(("y", dz, dy, 0, 0))

    def third(self, dz):
        depth, rows, cols, cores = self.place.dims
        terms = [self.get(("x", dz, 0, dx, 0)) for dx in range(1, cols)]
        terms += [self.get(("y", dz, dy, 0, 0)) for dy in range(1, rows)]
        if dz:
            if terms:
                self.add(self.place.at(dz, 0, 0), self.span(None), terms)
            self.put(("z", dz, 0, 0, 0))
            return None
        value = self.parts[self.place.me].astype(jnp.float32)
        for term in terms:
            value = value + term
        return value

    def finish(self):
        for c in self.sent:
            c.wait_send()


def experts_kernel(
    dims, seqs, width, own, resid, gate_hbm, up_hbm, down_hbm, out,
    held, parts, slots, gate, up, down, mine, load, send, recv, back_send, back_recv,
):
    place = Place(dims)
    depth, rows, cols, cores = dims
    count = math.prod(dims)
    plane = rows * cols * cores
    fills = [
        pltpu.make_async_copy(a, b, load.at[i])
        for i, (a, b) in enumerate(
            [(own, held.at[place.me]), (gate_hbm.at[0], gate), (up_hbm.at[0], up), (down_hbm.at[0], down), (resid, mine)]
        )
    ]
    for fill in fills:
        fill.start()
    place.greet()
    fills[0].wait()
    g = Gather(place, halves(held, held.shape[2]), send, recv)
    r = Reduce(place, parts, slots, back_send, back_recv)
    padded = held.shape[1]
    step = max(1, 192 // padded)
    while plane % step:
        step -= 1

    def serve(dz):
        base = ((place.spot[0] + dz) % depth) * plane
        extra = held.shape[2] - width
        lane = lax.broadcasted_iota(jnp.int32, (step * padded, extra), 1)
        pick = jnp.logical_or(lane == place.me, lane == place.me + count)
        for k in range(0, plane, step):
            some = held[pl.ds(base + k, step)].reshape(step * padded, held.shape[2])
            rows_in = some[:, :width]
            scale = jnp.sum(
                jnp.where(pick, some[:, width:].astype(jnp.float32), 0.0), axis=1, keepdims=True
            )
            gate_part = jnp.dot(rows_in, gate[...], preferred_element_type=jnp.float32)
            up_part = jnp.dot(rows_in, up[...], preferred_element_type=jnp.float32)
            hidden = (gate_part * jax.nn.sigmoid(gate_part) * up_part).astype(jnp.bfloat16)
            served = jnp.dot(hidden, down[...], preferred_element_type=jnp.float32) * scale
            parts[pl.ds(base + k, step)] = served.astype(jnp.bfloat16).reshape(step, padded, width)

    total = None
    for t in range(depth + 6):
        if t < depth:
            g.first(t)
        if 0 <= t - 1 < depth:
            g.second(t - 1)
        if 0 <= t - 2 < depth:
            g.third(t - 2)
        if 0 <= t - 3 < depth:
            g.fourth(t - 3)
            if t == 3:
                for fill in fills[1:]:
                    fill.wait()
            serve(t - 3)
            r.zeroth(t - 3)
        if 0 <= t - 4 < depth:
            r.first(t - 4)
        if 0 <= t - 5 < depth:
            r.second(t - 5)
        if 0 <= t - 6 < depth:
            value = r.third(t - 6)
            total = value if value is not None else total
    for dz in range(1, depth):
        total = total + r.get(("z", dz, 0, 0, 0))
    out[...] = (mine[...].astype(jnp.float32) + total[:seqs]).astype(out.dtype)
    g.finish()
    r.finish()


def experts(dims, block, resid, gate, up, down, collective):
    count = math.prod(dims)
    seqs, width = resid.shape
    messages = len(gather_names(dims))
    padded = block.shape[0]
    anywhere = pl.BlockSpec(memory_space=pl.ANY)
    return pl.pallas_call(
        functools.partial(experts_kernel, dims, seqs, width),
        out_shape=jax.ShapeDtypeStruct(resid.shape, resid.dtype),
        in_specs=[anywhere] * 5,
        out_specs=pl.BlockSpec(memory_space=pltpu.VMEM),
        scratch_shapes=[
            pltpu.VMEM((count,) + block.shape, block.dtype),
            pltpu.VMEM((count, padded, width), jnp.bfloat16),
            pltpu.VMEM((messages, padded, width), jnp.bfloat16),
            pltpu.VMEM(gate.shape[1:], gate.dtype),
            pltpu.VMEM(up.shape[1:], up.dtype),
            pltpu.VMEM(down.shape[1:], down.dtype),
            pltpu.VMEM(resid.shape, resid.dtype),
            pltpu.SemaphoreType.DMA((5,)),
        ] + [pltpu.SemaphoreType.DMA((messages,))] * 4,
        compiler_params=pltpu.CompilerParams(
            collective_id=collective, has_side_effects=True, vmem_limit_bytes=VMEM_LIMIT
        ),
        name="experts",
    )(block, resid, gate, up, down)


def rms_scale(values, gain):
    wide = values.astype(jnp.float32)
    scaled = wide * lax.rsqrt(jnp.mean(wide * wide, axis=-1, keepdims=True) + EPS)
    return (scaled * gain).astype(jnp.bfloat16)


def rotate(field, spots):
    half = field.shape[-1] // 2
    freqs = jnp.exp(-math.log(10000.0) * jnp.arange(half, dtype=jnp.float32) / half)
    angle = spots.astype(jnp.float32)[:, None] * freqs[None, :]
    cosine = jnp.cos(angle)[:, None, :]
    sine = jnp.sin(angle)[:, None, :]
    first = field[..., :half]
    second = field[..., half:]
    return jnp.concatenate(
        [first * cosine - second * sine, second * cosine + first * sine], axis=-1
    )


def shards(
    dims,
    tokens,
    positions,
    state,
    mix_gain,
    w_query,
    w_key,
    w_value,
    ret_gain,
    w_out,
    ffn_gain,
    routes,
    route_weights,
    expert_gate,
    expert_up,
    expert_down,
):
    seqs = tokens.shape[0]
    width = tokens.shape[1]
    heads = state.shape[1]
    head_k = state.shape[2]
    head_v = state.shape[3]
    normed_in = rms_scale(tokens, mix_gain)
    q_proj = jnp.dot(normed_in, w_query, preferred_element_type=jnp.float32).astype(jnp.bfloat16)
    k_proj = jnp.dot(normed_in, w_key, preferred_element_type=jnp.float32).astype(jnp.bfloat16)
    v_proj = jnp.dot(normed_in, w_value, preferred_element_type=jnp.float32).astype(jnp.bfloat16)
    queries = rotate(q_proj.astype(jnp.float32).reshape(seqs, heads, head_k), positions)
    key_rows = rotate(
        k_proj.astype(jnp.float32).reshape(seqs, heads, head_k), positions
    ) * head_k ** (-0.5)
    values = v_proj.astype(jnp.float32).reshape(seqs, heads, head_v)
    decays = 1.0 - jnp.exp2(-2.0 - jnp.arange(heads, dtype=jnp.float32))
    new_state = (
        decays[None, :, None, None] * state + key_rows[:, :, :, None] * values[:, :, None, :]
    )
    readout = jnp.einsum("thd,thdv->thv", queries, new_state, precision=lax.Precision.HIGHEST)
    centre = jnp.mean(readout, axis=-1, keepdims=True)
    variance = jnp.mean(jnp.square(readout - centre), axis=-1, keepdims=True)
    normed = ((readout - centre) * lax.rsqrt(variance + EPS)).reshape(
        seqs, heads * head_v
    ) * ret_gain
    mixed = normed.astype(jnp.bfloat16)
    attended = jnp.dot(
        mixed,
        gather_blocks(dims, w_out.T, 0).reshape(width, heads * head_v).T,
        preferred_element_type=jnp.float32,
    ).astype(jnp.bfloat16)
    resid = (tokens.astype(jnp.float32) + attended.astype(jnp.float32)).astype(jnp.bfloat16)
    normed_mid = rms_scale(resid, ffn_gain)
    count = lax.axis_size("ep")
    ids = jnp.arange(count, dtype=jnp.int32)
    wide_weights = jnp.sum(
        jnp.where(routes[:, :, None] == ids[None, None, :], route_weights[:, :, None], 0.0), axis=1
    )
    high = wide_weights.astype(jnp.bfloat16)
    low = (wide_weights - high.astype(jnp.float32)).astype(jnp.bfloat16)
    fill = -(-2 * count // 128) * 128 - 2 * count
    block = jnp.concatenate(
        [normed_mid, high, low, jnp.zeros((seqs, fill), jnp.bfloat16)], axis=1
    )
    block = jnp.pad(block, ((0, -(-seqs // PAD) * PAD - seqs), (0, 0)))
    result = experts(dims, block, resid, expert_gate, expert_up, expert_down, 1)
    return (result, new_state)


def solution(mesh):
    placed = (
        P("ep", None),
        P("ep"),
        P("ep", None, None, None),
        P(),
        P(),
        P(),
        P(),
        P(),
        P(None, "ep"),
        P(),
        P("ep", None),
        P("ep", None),
        P("ep", None, None),
        P("ep", None, None),
        P("ep", None, None),
    )
    return jax.shard_map(
        functools.partial(shards, layout_of(mesh)),
        mesh=mesh,
        in_specs=placed,
        out_specs=(P("ep", None), P("ep", None, None, None)),
        check_vma=False,
    )
```

```python
import functools
import math

import jax
import jax.numpy as jnp
from jax import lax
from jax.experimental import pallas as pl
from jax.experimental.pallas import tpu as pltpu
from jax.sharding import PartitionSpec as P

EPS = 1e-06
MESH = pl.DeviceIdType.MESH
PAD = 8
VMEM_LIMIT = 64 * 1024 * 1024 - 128 * 1024


def layout_of(mesh):
    devices = list(mesh.devices.flat)
    count = len(devices)
    try:
        far = [max(d.coords[i] for d in devices) - min(d.coords[i] for d in devices) + 1 for i in range(3)]
        cores = count // (far[0] * far[1] * far[2])
        if cores * far[0] * far[1] * far[2] == count and cores >= 1:
            return (far[2], far[1], far[0], cores)
    except (AttributeError, TypeError, IndexError):
        pass
    cores = 2 if count % 2 == 0 else 1
    chips = count // cores
    side = 1
    while (side * 2) ** 2 * 4 <= chips and chips % ((side * 2) ** 2) == 0:
        side *= 2
    return (chips // (side * side), side, side, cores)


class Place:
    def __init__(self, dims):
        self.dims = dims
        depth, rows, cols, cores = dims
        me = lax.axis_index("ep")
        self.me = me
        self.spot = (
            me // (rows * cols * cores),
            (me // (cols * cores)) % rows,
            (me // cores) % cols,
            me % cores,
        )

    def at(self, dz, dy, dx, dc=0):
        total = 0
        for size, here, move in zip(self.dims, self.spot, (dz, dy, dx, dc)):
            total = total * size + self.moved(size, here, move)
        return total

    @staticmethod
    def moved(size, here, move):
        if not move % size:
            return here
        if size & (size - 1):
            return (here + move) % size
        bit = 1
        there = here
        while bit < size:
            if abs(move) & bit:
                there = there + bit - 2 * bit * ((here // bit) % 2)
            bit *= 2
        return there

    def greet(self, corners=False):
        depth, rows, cols, cores = self.dims
        moves = [(d, 0, 0, 0) for d in range(1, depth)]
        moves += [(0, d, 0, 0) for d in range(1, rows)]
        moves += [(0, 0, d, 0) for d in range(1, cols)]
        if corners:
            moves += [(0, dy, dx, 0) for dy in range(1, rows) for dx in range(1, cols)]
        moves += [(0, 0, 0, d) for d in range(1, cores)]
        barrier = pltpu.get_barrier_semaphore()
        for move in moves:
            pl.semaphore_signal(barrier, inc=1, device_id=(self.at(*move),), device_id_type=MESH)
        pl.semaphore_wait(barrier, len(moves))


def gather_names(dims):
    depth, rows, cols, cores = dims
    names = []
    for dz in range(depth):
        if dz:
            names.append(("z", dz, 0, 0, 0))
        for dx in range(1, cols):
            names.append(("x", dz, 0, dx, 0))
        for dy in range(1, rows):
            names.append(("y", dz, dy, 0, 0))
            for dx in range(1, cols):
                names.append(("p", dz, dy, dx, 0))
                names.append(("q", dz, dy, dx, 0))
        for dy in range(rows):
            for dx in range(cols):
                for dc in range(1, cores):
                    names.append(("c", dz, dy, dx, dc))
    return {name: i for i, name in enumerate(names)}


class Gather:
    def __init__(self, place, view, send, recv):
        self.place, self.view, self.send, self.recv = place, view, send, recv
        self.names = gather_names(place.dims)
        self.sent = []

    def copy(self, name):
        kind, dz, dy, dx, dc = name
        m = self.names[name]
        back = {"z": (-dz, 0, 0, 0), "x": (0, 0, -dx, 0), "y": (0, -dy, 0, 0)}
        back.update({"p": (0, -dy, 0, 0), "q": (0, 0, -dx, 0), "c": (0, 0, 0, -dc)})
        return m, {"p": 0, "q": 1}.get(kind), self.place.at(*back[kind])

    def put(self, name, held):
        m, half, target = self.copy(name)
        ref = self.view(self.place.at(*held), half)
        c = pltpu.make_async_remote_copy(
            src_ref=ref, dst_ref=ref, send_sem=self.send.at[m], recv_sem=self.recv.at[m],
            device_id=(target,), device_id_type=MESH,
        )
        c.start()
        self.sent.append(c)

    def get(self, name):
        m, half, target = self.copy(name)
        ref = self.view(self.place.at(*name[1:]), half)
        pltpu.make_async_remote_copy(
            src_ref=ref, dst_ref=ref, send_sem=self.send.at[m], recv_sem=self.recv.at[m],
            device_id=(target,), device_id_type=MESH,
        ).wait_recv()

    def mates(self, dz, dy, dx):
        for dc in range(1, self.place.dims[3]):
            self.put(("c", dz, dy, dx, dc), (dz, dy, dx, 0))

    def first(self, dz):
        depth, rows, cols, cores = self.place.dims
        if dz == 0:
            for d in range(1, depth):
                self.put(("z", d, 0, 0, 0), (0, 0, 0, 0))
        else:
            self.get(("z", dz, 0, 0, 0))
        for dx in range(1, cols):
            self.put(("x", dz, 0, dx, 0), (dz, 0, 0, 0))
        for dy in range(1, rows):
            self.put(("y", dz, dy, 0, 0), (dz, 0, 0, 0))
        self.mates(dz, 0, 0)

    def second(self, dz):
        depth, rows, cols, cores = self.place.dims
        for dx in range(1, cols):
            self.get(("x", dz, 0, dx, 0))
            for dy in range(1, rows):
                self.put(("p", dz, dy, dx, 0), (dz, 0, dx, 0))
            self.mates(dz, 0, dx)
        for dy in range(1, rows):
            self.get(("y", dz, dy, 0, 0))
            for dx in range(1, cols):
                self.put(("q", dz, dy, dx, 0), (dz, dy, 0, 0))
            self.mates(dz, dy, 0)

    def third(self, dz):
        depth, rows, cols, cores = self.place.dims
        for dy in range(1, rows):
            for dx in range(1, cols):
                self.get(("p", dz, dy, dx, 0))
                self.get(("q", dz, dy, dx, 0))
                self.mates(dz, dy, dx)

    def fourth(self, dz):
        depth, rows, cols, cores = self.place.dims
        for dy in range(rows):
            for dx in range(cols):
                for dc in range(1, cores):
                    self.get(("c", dz, dy, dx, dc))

    def finish(self):
        for c in self.sent:
            c.wait_send()


def halves(ref, width):
    cut = -(-width // 256) * 128
    spans = {None: (0, width), 0: (0, cut), 1: (cut, width - cut)}

    def view(index, half):
        start, size = spans[half]
        return ref.at[index, :, pl.ds(start, size)]

    return view


def retain_kernel(
    dims, sizes, own, normed, wq_hbm, wk_hbm, wv_hbm, cosine, sine, gain, state_hbm,
    out, key_out, value_out,
    wq, wk, wv, state, flip, qcols, kcols, values, decay, readout, lines, mixed, attended, back,
    load, wload, sload, send, recv,
):
    heads, head_k, head_v = sizes
    place = Place(dims)
    seqs = normed.shape[0]
    depth, rows, cols, cores = dims
    names = retain_names(dims)

    def slot(dz, dc):
        return place.moved(depth, place.spot[0], dz) * cores + place.moved(cores, place.spot[3], dc)

    def remote(name, src, dst, target):
        m = names[name]
        return pltpu.make_async_remote_copy(
            src_ref=src, dst_ref=dst, send_sem=send.at[m], recv_sem=recv.at[m],
            device_id=(place.at(*target),), device_id_type=MESH,
        )

    fill = pltpu.make_async_copy(own, lines.at[slot(0, 0)], load)
    fill.start()
    weights = [
        pltpu.make_async_copy(src, dst, wload.at[i])
        for i, (src, dst) in enumerate([(wq_hbm, wq), (wk_hbm, wk), (wv_hbm, wv)])
    ]
    for copy in weights:
        copy.start()
    taken = pltpu.make_async_copy(state_hbm, state, sload)
    taken.start()
    place.greet(corners=True)
    fill.wait()
    sent = []

    def put(*args):
        copy = remote(*args)
        copy.start()
        sent.append(copy)

    for dz in range(1, depth):
        put(("z", dz), lines.at[slot(0, 0)], lines.at[slot(0, 0)], (-dz, 0, 0, 0))
    for dc in range(1, cores):
        put(("c", 0, dc), lines.at[slot(0, 0)], lines.at[slot(0, 0)], (0, 0, 0, -dc))

    def rotated(field):
        lane = lax.broadcasted_iota(jnp.int32, field.shape, 1) % head_k
        total = field.shape[1]
        ahead = pltpu.roll(field, total - head_k // 2, 1)
        behind = pltpu.roll(field, head_k // 2, 1)
        return field * cosine[...] + jnp.where(lane < head_k // 2, -ahead, behind) * sine[...]

    def columns(field, target):
        flip[...] = jnp.zeros_like(flip)
        flip[pl.ds(0, seqs), :] = field
        target[...] = flip[...].T

    def project(weight):
        part = jnp.dot(normed[...], weight[...], preferred_element_type=jnp.float32)
        return part.astype(jnp.bfloat16).astype(jnp.float32)

    def queries():
        weights[0].wait()
        columns(rotated(project(wq)), qcols)

    def keys():
        weights[1].wait()
        key_out[...] = rotated(project(wk)) * head_k ** (-0.5)
        columns(key_out[...], kcols)

    def others():
        weights[2].wait()
        part = project(wv)
        value_out[...] = part
        for h in range(heads):
            values[:, h, :] = part[:, h * head_v : (h + 1) * head_v]
            decay[pl.ds(h * head_k, head_k), :] = jnp.full((head_k, head_v), 1.0 - 2.0 ** (-2.0 - h), jnp.float32)
        taken.wait()

    def span(start, stop):
        def one(t, carry):
            lane = lax.broadcasted_iota(jnp.int32, qcols.shape, 1)
            query = jnp.sum(jnp.where(lane == t, qcols[...], 0.0), axis=1, keepdims=True)
            key = jnp.sum(jnp.where(lane == t, kcols[...], 0.0), axis=1, keepdims=True)
            value = values[t]
            outer = key.reshape(heads, head_k, 1) * value.reshape(heads, 1, head_v)
            fresh = decay[...] * state[t] + outer.reshape(heads * head_k, head_v)
            readout[t] = jnp.sum((query * fresh).reshape(heads, head_k, head_v), axis=1)
            return carry

        lax.fori_loop(start, stop, one, 0)

    def close():
        for h in range(heads):
            read = readout[:, h, :]
            apart = read - jnp.mean(read, axis=1, keepdims=True)
            variance = jnp.mean(apart * apart, axis=1, keepdims=True)
            lanes = pl.ds(h * head_v, head_v)
            mixed[0, pl.ds(0, seqs), lanes] = (apart * lax.rsqrt(variance + EPS) * gain[:, lanes]).astype(mixed.dtype)

    queries()
    keys()
    others()
    span(0, seqs)
    mixed[0] = jnp.zeros(mixed.shape[1:], mixed.dtype)
    close()
    moves = [(dy, dx) for dy in range(rows) for dx in range(cols)]
    for i, (dy, dx) in enumerate(moves):
        if i:
            put(("m", dy, dx), mixed.at[0], mixed.at[i], (0, -dy, -dx, 0))
    for dz in range(1, depth):
        held = lines.at[slot(dz, 0)]
        remote(("z", dz), held, held, (-dz, 0, 0, 0)).wait_recv()
        for dc in range(1, cores):
            put(("c", dz, dc), held, held, (0, 0, 0, -dc))
    for i, (dy, dx) in enumerate(moves):
        if i:
            remote(("m", dy, dx), mixed.at[0], mixed.at[i], (0, -dy, -dx, 0)).wait_recv()
    for dz in range(depth):
        for dc in range(1, cores):
            held = lines.at[slot(dz, dc)]
            remote(("c", dz, dc), held, held, (0, 0, 0, -dc)).wait_recv()
    tall = mixed.shape[1]
    product = lax.dot_general(
        mixed[...].reshape(len(moves) * tall, mixed.shape[2]),
        lines[...].reshape(-1, lines.shape[2]),
        (((1,), (1,)), ((), ())),
        preferred_element_type=jnp.float32,
    )
    attended[...] = product.astype(attended.dtype).reshape(attended.shape)
    for i, (dy, dx) in enumerate(moves):
        if i:
            put(("r", dy, dx), attended.at[i], back.at[i], (0, dy, dx, 0))
    for i, (dy, dx) in enumerate(moves):
        origin = place.moved(rows, place.spot[1], -dy) * cols + place.moved(cols, place.spot[2], -dx)
        if i:
            remote(("r", dy, dx), attended.at[i], back.at[i], (0, dy, dx, 0)).wait_recv()
        out[origin] = back[i] if i else attended[0]
    for copy in sent:
        copy.wait_send()


def retain_names(dims):
    depth, rows, cols, cores = dims
    names = [("z", dz) for dz in range(1, depth)]
    names += [("c", dz, dc) for dz in range(depth) for dc in range(1, cores)]
    names += [(k, dy, dx) for k in "mr" for dy in range(rows) for dx in range(cols) if dy or dx]
    return {name: i for i, name in enumerate(names)}


def retain(dims, sizes, block, normed, wq, wk, wv, cosine, sine, gain, state, collective):
    heads, head_k, head_v = sizes
    depth, rows, cols, cores = dims
    messages = len(retain_names(dims))
    seqs = normed.shape[0]
    flat = (seqs, heads * head_k, head_v)
    anywhere = pl.BlockSpec(memory_space=pl.ANY)
    here = pl.BlockSpec(memory_space=pltpu.VMEM)
    across = -(-seqs // 128) * 128
    tall = -(-seqs // PAD) * PAD
    some = depth * cores * block.shape[0]
    plane = rows * cols
    return pl.pallas_call(
        functools.partial(retain_kernel, dims, sizes),
        out_shape=(
            jax.ShapeDtypeStruct((plane, tall, some), jnp.bfloat16),
            jax.ShapeDtypeStruct((seqs, heads * head_k), jnp.float32),
            jax.ShapeDtypeStruct((seqs, heads * head_v), jnp.float32),
        ),
        in_specs=[anywhere, here, anywhere, anywhere, anywhere, here, here, here, anywhere],
        out_specs=(here, here, here),
        scratch_shapes=[
            pltpu.VMEM(wq.shape, wq.dtype),
            pltpu.VMEM(wk.shape, wk.dtype),
            pltpu.VMEM(wv.shape, wv.dtype),
            pltpu.VMEM(flat, jnp.float32),
            pltpu.VMEM((across, heads * head_k), jnp.float32),
            pltpu.VMEM((heads * head_k, across), jnp.float32),
            pltpu.VMEM((heads * head_k, across), jnp.float32),
            pltpu.VMEM((seqs, heads, head_v), jnp.float32),
            pltpu.VMEM((heads * head_k, head_v), jnp.float32),
            pltpu.VMEM((seqs, heads, head_v), jnp.float32),
            pltpu.VMEM((depth * cores,) + block.shape, block.dtype),
            pltpu.VMEM((plane, tall, heads * head_v), jnp.bfloat16),
            pltpu.VMEM((plane, tall, some), jnp.bfloat16),
            pltpu.VMEM((plane, tall, some), jnp.bfloat16),
            pltpu.SemaphoreType.DMA,
            pltpu.SemaphoreType.DMA((3,)),
            pltpu.SemaphoreType.DMA,
            pltpu.SemaphoreType.DMA((messages,)),
            pltpu.SemaphoreType.DMA((messages,)),
        ],
        compiler_params=pltpu.CompilerParams(
            collective_id=collective, has_side_effects=True, vmem_limit_bytes=VMEM_LIMIT
        ),
        name="retain",
    )(block, normed, wq, wk, wv, cosine, sine, gain, state.reshape(flat))


class Reduce:
    def __init__(self, place, parts, slots, send, recv):
        self.place, self.parts, self.slots, self.send, self.recv = place, parts, slots, send, recv
        self.names = gather_names(place.dims)
        self.sent = []
        self.width = parts.shape[2]

    def span(self, half):
        cut = self.width // 2
        return {None: pl.ds(0, self.width), 0: pl.ds(0, cut), 1: pl.ds(cut, self.width - cut)}[half]

    def copy(self, name):
        kind, dz, dy, dx, dc = name
        m = self.names[name]
        ahead = {"z": (dz, 0, 0, 0), "x": (0, 0, dx, 0), "y": (0, dy, 0, 0)}
        ahead.update({"p": (0, dy, 0, 0), "q": (0, 0, dx, 0), "c": (0, 0, 0, dc)})
        cols = self.span({"p": 0, "q": 1}.get(kind))
        return pltpu.make_async_remote_copy(
            src_ref=self.parts.at[self.place.at(dz, dy, dx, dc), :, cols],
            dst_ref=self.slots.at[m, :, cols],
            send_sem=self.send.at[m], recv_sem=self.recv.at[m],
            device_id=(self.place.at(*ahead[kind]),), device_id_type=MESH,
        )

    def put(self, name):
        c = self.copy(name)
        c.start()
        self.sent.append(c)

    def get(self, name):
        kind = name[0]
        self.copy(name).wait_recv()
        cols = self.span({"p": 0, "q": 1}.get(kind))
        return self.slots[self.names[name], :, cols].astype(jnp.float32)

    def add(self, index, cols, terms):
        value = self.parts[index, :, cols].astype(jnp.float32)
        for term in terms:
            value = value + term
        self.parts[index, :, cols] = value.astype(self.parts.dtype)

    def zeroth(self, dz):
        depth, rows, cols, cores = self.place.dims
        order = sorted(((dy, dx) for dy in range(rows) for dx in range(cols)), key=lambda o: (not o[0]) + (not o[1]))
        for dy, dx in order:
            for dc in range(1, cores):
                self.put(("c", dz, dy, dx, dc))

    def first(self, dz):
        depth, rows, cols, cores = self.place.dims
        order = sorted(((dy, dx) for dy in range(rows) for dx in range(cols)), key=lambda o: (not o[0]) + (not o[1]))
        for dy, dx in order:
            terms = [self.get(("c", dz, dy, dx, dc)) for dc in range(1, cores)]
            if terms:
                self.add(self.place.at(dz, dy, dx), self.span(None), terms)
            if dy and dx:
                self.put(("p", dz, dy, dx, 0))
                self.put(("q", dz, dy, dx, 0))

    def second(self, dz):
        depth, rows, cols, cores = self.place.dims
        for dx in range(1, cols):
            terms = [self.get(("p", dz, dy, dx, 0)) for dy in range(1, rows)]
            if terms:
                self.add(self.place.at(dz, 0, dx), self.span(0), terms)
            self.put(("x", dz, 0, dx, 0))
        for dy in range(1, rows):
            terms = [self.get(("q", dz, dy, dx, 0)) for dx in range(1, cols)]
            if terms:
                self.add(self.place.at(dz, dy, 0), self.span(1), terms)
            self.put(("y", dz, dy, 0, 0))

    def third(self, dz):
        depth, rows, cols, cores = self.place.dims
        terms = [self.get(("x", dz, 0, dx, 0)) for dx in range(1, cols)]
        terms += [self.get(("y", dz, dy, 0, 0)) for dy in range(1, rows)]
        if dz:
            if terms:
                self.add(self.place.at(dz, 0, 0), self.span(None), terms)
            self.put(("z", dz, 0, 0, 0))
            return None
        value = self.parts[self.place.me].astype(jnp.float32)
        for term in terms:
            value = value + term
        return value

    def finish(self):
        for c in self.sent:
            c.wait_send()


def experts_kernel(
    dims, seqs, width, own, resid, gate_hbm, up_hbm, down_hbm, out,
    held, parts, slots, gate, up, down, mine, load, send, recv, back_send, back_recv,
):
    place = Place(dims)
    depth, rows, cols, cores = dims
    count = math.prod(dims)
    plane = rows * cols * cores
    fills = [
        pltpu.make_async_copy(a, b, load.at[i])
        for i, (a, b) in enumerate(
            [(own, held.at[place.me]), (gate_hbm.at[0], gate), (up_hbm.at[0], up), (down_hbm.at[0], down), (resid, mine)]
        )
    ]
    for fill in fills:
        fill.start()
    place.greet()
    fills[0].wait()
    g = Gather(place, halves(held, held.shape[2]), send, recv)
    r = Reduce(place, parts, slots, back_send, back_recv)
    padded = held.shape[1]
    step = max(1, 192 // padded)
    while plane % step:
        step -= 1

    def serve(dz):
        base = place.moved(depth, place.spot[0], dz) * plane
        extra = held.shape[2] - width
        lane = lax.broadcasted_iota(jnp.int32, (step * padded, extra), 1)
        pick = jnp.logical_or(lane == place.me, lane == place.me + count)
        for k in range(0, plane, step):
            some = held[pl.ds(base + k, step)].reshape(step * padded, held.shape[2])
            rows_in = some[:, :width]
            scale = jnp.sum(
                jnp.where(pick, some[:, width:].astype(jnp.float32), 0.0), axis=1, keepdims=True
            )
            gate_part = jnp.dot(rows_in, gate[...], preferred_element_type=jnp.float32)
            up_part = jnp.dot(rows_in, up[...], preferred_element_type=jnp.float32)
            hidden = (gate_part * jax.nn.sigmoid(gate_part) * up_part).astype(jnp.bfloat16)
            served = jnp.dot(hidden, down[...], preferred_element_type=jnp.float32) * scale
            parts[pl.ds(base + k, step)] = served.astype(jnp.bfloat16).reshape(step, padded, width)

    total = None
    for t in range(depth + 6):
        if t < depth:
            g.first(t)
        if 0 <= t - 1 < depth:
            g.second(t - 1)
        if 0 <= t - 2 < depth:
            g.third(t - 2)
        if 0 <= t - 3 < depth:
            g.fourth(t - 3)
            if t == 3:
                for fill in fills[1:]:
                    fill.wait()
            serve(t - 3)
            r.zeroth(t - 3)
        if 0 <= t - 4 < depth:
            r.first(t - 4)
        if 0 <= t - 5 < depth:
            r.second(t - 5)
        if 0 <= t - 6 < depth:
            value = r.third(t - 6)
            total = value if value is not None else total
    for dz in range(1, depth):
        total = total + r.get(("z", dz, 0, 0, 0))
    out[...] = (mine[...].astype(jnp.float32) + total[:seqs]).astype(out.dtype)
    g.finish()
    r.finish()


def experts(dims, block, resid, gate, up, down, collective):
    count = math.prod(dims)
    seqs, width = resid.shape
    messages = len(gather_names(dims))
    padded = block.shape[0]
    anywhere = pl.BlockSpec(memory_space=pl.ANY)
    return pl.pallas_call(
        functools.partial(experts_kernel, dims, seqs, width),
        out_shape=jax.ShapeDtypeStruct(resid.shape, resid.dtype),
        in_specs=[anywhere] * 5,
        out_specs=pl.BlockSpec(memory_space=pltpu.VMEM),
        scratch_shapes=[
            pltpu.VMEM((count,) + block.shape, block.dtype),
            pltpu.VMEM((count, padded, width), jnp.bfloat16),
            pltpu.VMEM((messages, padded, width), jnp.bfloat16),
            pltpu.VMEM(gate.shape[1:], gate.dtype),
            pltpu.VMEM(up.shape[1:], up.dtype),
            pltpu.VMEM(down.shape[1:], down.dtype),
            pltpu.VMEM(resid.shape, resid.dtype),
            pltpu.SemaphoreType.DMA((5,)),
        ] + [pltpu.SemaphoreType.DMA((messages,))] * 4,
        compiler_params=pltpu.CompilerParams(
            collective_id=collective, has_side_effects=True, vmem_limit_bytes=VMEM_LIMIT
        ),
        name="experts",
    )(block, resid, gate, up, down)


def rms_scale(values, gain):
    wide = values.astype(jnp.float32)
    scaled = wide * lax.rsqrt(jnp.mean(wide * wide, axis=-1, keepdims=True) + EPS)
    return (scaled * gain).astype(jnp.bfloat16)


def padded_rows(rows):
    return jnp.pad(rows, ((0, -(-rows.shape[0] // PAD) * PAD - rows.shape[0]), (0, 0)))


def shards(
    dims,
    tokens,
    positions,
    state,
    mix_gain,
    w_query,
    w_key,
    w_value,
    ret_gain,
    w_out,
    ffn_gain,
    routes,
    route_weights,
    expert_gate,
    expert_up,
    expert_down,
):
    seqs = tokens.shape[0]
    width = tokens.shape[1]
    heads = state.shape[1]
    head_k = state.shape[2]
    head_v = state.shape[3]
    normed_in = rms_scale(tokens, mix_gain)
    half = head_k // 2
    freqs = jnp.exp(-math.log(10000.0) * jnp.arange(half, dtype=jnp.float32) / half)
    angle = positions.astype(jnp.float32)[:, None] * jnp.tile(freqs, 2 * heads)[None, :]
    columns, key_rows, values = retain(
        dims, (heads, head_k, head_v), w_out.T, normed_in, w_query, w_key, w_value,
        jnp.cos(angle), jnp.sin(angle), ret_gain.reshape(1, -1), state, 0,
    )
    key_rows = key_rows.reshape(seqs, heads, head_k)
    values = values.reshape(seqs, heads, head_v)
    decays = 1.0 - jnp.exp2(-2.0 - jnp.arange(heads, dtype=jnp.float32))
    new_state = (
        decays[None, :, None, None] * state + key_rows[:, :, :, None] * values[:, :, None, :]
    )
    count = lax.axis_size("ep")
    columns = columns[:, :seqs].reshape(dims[1] * dims[2], seqs, dims[0], -1)
    attended = jnp.transpose(columns, (1, 2, 0, 3)).reshape(seqs, width)
    resid = (tokens.astype(jnp.float32) + attended.astype(jnp.float32)).astype(jnp.bfloat16)
    normed_mid = rms_scale(resid, ffn_gain)
    ids = jnp.arange(count, dtype=jnp.int32)
    wide_weights = jnp.sum(
        jnp.where(routes[:, :, None] == ids[None, None, :], route_weights[:, :, None], 0.0), axis=1
    )
    high = wide_weights.astype(jnp.bfloat16)
    low = (wide_weights - high.astype(jnp.float32)).astype(jnp.bfloat16)
    fill = -(-2 * count // 128) * 128 - 2 * count
    block = jnp.concatenate(
        [normed_mid, high, low, jnp.zeros((seqs, fill), jnp.bfloat16)], axis=1
    )
    block = padded_rows(block)
    result = experts(dims, block, resid, expert_gate, expert_up, expert_down, 1)
    return (result, new_state)


def solution(mesh):
    placed = (
        P("ep", None),
        P("ep"),
        P("ep", None, None, None),
        P(),
        P(),
        P(),
        P(),
        P(),
        P(None, "ep"),
        P(),
        P("ep", None),
        P("ep", None),
        P("ep", None, None),
        P("ep", None, None),
        P("ep", None, None),
    )
    return jax.shard_map(
        functools.partial(shards, layout_of(mesh)),
        mesh=mesh,
        in_specs=placed,
        out_specs=(P("ep", None), P("ep", None, None, None)),
        check_vma=False,
    )
```
